32 devices in a mesh: fs: 4 (over y, x), tp: 8 (over z, core).
Axes of the slice: x: 2, y: 2, z: 4, core: 2. Of those that a mesh axis runs over, the one named last changes fastest.
Arguments:
- features: bfloat16 [8192, 2048], P('fs', 'tp'), may hold values from -6 to 6
- gate_cotangent: bfloat16 [8192, 4096], P('fs', 'tp'), may hold values from -0.059814453 to 0.059814453
- gate_basis: bfloat16 [2048, 128], replicated, may hold values from -0.125 to 0.125
- gate_master: float32 [2048, 4096], P('fs', 'tp'), may hold values from -6 to 6
- gate_first: float32 [128, 4096], P('fs', 'tp'), may hold values from -144 to 144
- gate_second: float32 [128, 4096], P('fs', 'tp'), may hold values from 0.2 to 4
- input_cotangent: bfloat16 [8192, 4096], P('fs', 'tp'), may hold values from -0.059814453 to 0.059814453
- input_basis: bfloat16 [2048, 128], replicated, may hold values from -0.125 to 0.125
- input_master: float32 [2048, 4096], P('fs', 'tp'), may hold values from -6 to 6
- input_first: float32 [128, 4096], P('fs', 'tp'), may hold values from -144 to 144
- input_second: float32 [128, 4096], P('fs', 'tp'), may hold values from 0.2 to 4
- state_cotangent: bfloat16 [8192, 1024], P('fs', 'tp'), may hold values from -0.059814453 to 0.059814453
- state_basis: bfloat16 [2048, 128], replicated, may hold values from -0.125 to 0.125
- state_master: float32 [2048, 1024], P('fs', 'tp'), may hold values from -6 to 6
- state_first: float32 [128, 1024], P('fs', 'tp'), may hold values from -144 to 144
- state_second: float32 [128, 1024], P('fs', 'tp'), may hold values from 0.2 to 4
Outputs:
- gate_update: float32 [2048, 4096], P('fs', 'tp')
- gate_master_next: float32 [2048, 4096], P('fs', 'tp')
- gate_first_next: float32 [128, 4096], P('fs', 'tp')
- gate_second_next: float32 [128, 4096], P('fs', 'tp')
- gate_copy: bfloat16 [2048, 4096], P(None, 'tp')
- input_update: float32 [2048, 4096], P('fs', 'tp')
- input_master_next: float32 [2048, 4096], P('fs', 'tp')
- input_first_next: float32 [128, 4096], P('fs', 'tp')
- input_second_next: float32 [128, 4096], P('fs', 'tp')
- input_copy: bfloat16 [2048, 4096], P(None, 'tp')
- state_update: float32 [2048, 1024], P('fs', 'tp')
- state_master_next: float32 [2048, 1024], P('fs', 'tp')
- state_first_next: float32 [128, 1024], P('fs', 'tp')
- state_second_next: float32 [128, 1024], P('fs', 'tp')
- state_copy: bfloat16 [2048, 1024], P(None, 'tp')
The draws below stay inside these ranges and needn't reach their ends.
All inputs are finite; a program needn't handle non-finite values.
Results may differ from the reference program's by a relative error of at most 0.001.
Values may be sent and summed in bfloat16 or wider, within the bound.
A program may use at most 64 MiB of HBM per device.

```python
import math
import jax
import jax.numpy as jnp
from jax import lax

D = 2048
INNER = 4096
STATE_COLS = 1024
RANK = 128
TOKENS = 8192


def rising_moment(key, rows, columns):
    base = jnp.clip(jax.random.normal(key, (rows, columns), jnp.float32), -4.0, 4.0)
    row_pos = jnp.arange(rows, dtype=jnp.float32) / rows
    col_pos = jnp.arange(columns, dtype=jnp.float32) / columns
    growth = math.log(3.0)
    return base * jnp.exp(growth * (row_pos[:, None] + col_pos[None, :]))


def draw_gate_first(key, part):
    return rising_moment(jax.random.fold_in(key, 11), RANK, INNER)


def draw_input_first(key, part):
    return rising_moment(jax.random.fold_in(key, 12), RANK, INNER)


def draw_state_first(key, part):
    return rising_moment(jax.random.fold_in(key, 13), RANK, STATE_COLS)


def levels(key, dims, pieces, least, top_value):
    gain = 1.0
    for axis_at, shards_of in pieces:
        steps = jax.random.uniform(jax.random.fold_in(jax.random.fold_in(key, 6), axis_at), (shards_of,), jnp.float32, least / len(pieces), top_value / len(pieces))
        gain = gain * jnp.repeat(jnp.exp(steps), dims[axis_at] // shards_of).reshape((-1,) + (1,) * (len(dims) - 1 - axis_at))
    return gain


def gaussian(rng, extent, width, bound, cuts=(), kind=jnp.bfloat16):
    level = levels(rng, extent, cuts, -0.22, 0.18) if cuts else 1.0
    entries = jax.random.normal(rng, extent, jnp.float32) * width * level
    return jnp.minimum(jnp.maximum(entries, -bound), bound).astype(kind)


def setup_inputs(seed: int = 0) -> dict:
    key_of = jax.random.split(jax.random.key(seed), 17)
    return {
        "features": gaussian(key_of[0], (TOKENS, D), 1.0, 6.0, ((0, 4), (1, 8))),
        "gate_cotangent": gaussian(key_of[1], (TOKENS, INNER), 0.01, 0.059814453, ((0, 4), (1, 8))),
        "gate_basis": gaussian(key_of[2], (D, RANK), D ** -0.5, 0.125),
        "gate_master": gaussian(key_of[3], (D, INNER), 1.0, 6.0, ((0, 4), (1, 8)), jnp.float32),
        "gate_first": draw_gate_first(jax.random.fold_in(key_of[16], 71), 0),
        "gate_second": jnp.clip(jnp.exp(math.log(4.0) - 2.9957323 * jax.random.uniform(key_of[5], (RANK, INNER), jnp.float32) ** levels(key_of[5], (RANK, INNER), ((0, 4), (1, 8)), -0.2, 0.2)), 0.2, 4.0),
        "input_cotangent": gaussian(key_of[6], (TOKENS, INNER), 0.01, 0.059814453, ((0, 4), (1, 8))),
        "input_basis": gaussian(key_of[7], (D, RANK), D ** -0.5, 0.125),
        "input_master": gaussian(key_of[8], (D, INNER), 1.0, 6.0, ((0, 4), (1, 8)), jnp.float32),
        "input_first": draw_input_first(jax.random.fold_in(key_of[16], 71), 0),
        "input_second": jnp.clip(jnp.exp(math.log(4.0) - 2.9957323 * jax.random.uniform(key_of[10], (RANK, INNER), jnp.float32) ** levels(key_of[10], (RANK, INNER), ((0, 4), (1, 8)), -0.2, 0.2)), 0.2, 4.0),
        "state_cotangent": gaussian(key_of[11], (TOKENS, STATE_COLS), 0.01, 0.059814453, ((0, 4), (1, 8))),
        "state_basis": gaussian(key_of[12], (D, RANK), D ** -0.5, 0.125),
        "state_master": gaussian(key_of[13], (D, STATE_COLS), 1.0, 6.0, ((0, 4), (1, 8)), jnp.float32),
        "state_first": draw_state_first(jax.random.fold_in(key_of[16], 71), 0),
        "state_second": jnp.clip(jnp.exp(math.log(4.0) - 2.9957323 * jax.random.uniform(key_of[15], (RANK, STATE_COLS), jnp.float32) ** levels(key_of[15], (RANK, STATE_COLS), ((0, 4), (1, 8)), -0.2, 0.2)), 0.2, 4.0),
    }


def one_matrix(features, cotangent, basis, master, first, second):
    gradient = jnp.dot(features.T, cotangent, preferred_element_type=jnp.float32)
    basis_wide = basis.astype(jnp.float32)
    projected = jnp.dot(basis_wide.T, gradient, precision=lax.Precision.HIGHEST)
    first_next = 0.8 * first + 0.2 * projected
    second_next = 0.9 * second + 0.1 * projected * projected
    direction = first_next / jnp.sqrt(second_next)
    scale = lax.rsqrt(jnp.mean(direction * direction) + 1e-06)
    update = jnp.dot(basis_wide, direction, precision=lax.Precision.HIGHEST) * scale
    master_next = master - 0.05 * update
    return (update, master_next, first_next, second_next, master_next.astype(jnp.bfloat16))

def reference(features, gate_cotangent, gate_basis, gate_master, gate_first, gate_second, input_cotangent, input_basis, input_master, input_first, input_second, state_cotangent, state_basis, state_master, state_first, state_second):
    gate_out = one_matrix(features, gate_cotangent, gate_basis, gate_master, gate_first, gate_second)
    input_out = one_matrix(features, input_cotangent, input_basis, input_master, input_first, input_second)
    state_out = one_matrix(features, state_cotangent, state_basis, state_master, state_first, state_second)
    return (gate_out[0], gate_out[1], gate_out[2], gate_out[3], gate_out[4], input_out[0], input_out[1], input_out[2], input_out[3], input_out[4], state_out[0], state_out[1], state_out[2], state_out[3], state_out[4])
```

```python
import functools

import jax
import jax.numpy as jnp
from jax import lax
from jax.experimental import pallas as pl
from jax.experimental.pallas import tpu as pltpu
from jax.sharding import PartitionSpec as P

MESH = pl.DeviceIdType.MESH
PIECES = 4
SKEW = 2
F32, BF16 = jnp.float32, jnp.bfloat16


def kernel(n, tp, *refs):
    feat_in = refs[0]
    cot_in, basis_in, master_in, first_in, second_in = (refs[1 + i : 16 : 5] for i in range(5))
    upd_out, mas_out, fir_out, sec_out, cop_out = (refs[16 + i : 31 : 5] for i in range(5))
    (feat, fsib, cot, basis, master, first, second, parts, up_in, dn_in, up_snd, dn_snd,
     tot, sib, proj, rs_in, direction, sums, upd, mas, fir, sec, cop,
     load_sem, store_sem, z_send, z_recv, sib_send, sib_recv, rs_send, rs_recv,
     ag_send, ag_recv, sq_send, sq_recv, bulk_send, bulk_recv) = (
        refs[31], refs[32], refs[33:36], refs[36:39], refs[39:42], refs[42:45], refs[45:48],
        *refs[48:53], refs[53], refs[54], refs[55:58], refs[58:61], refs[61:64], refs[64],
        refs[65:68], refs[68:71], refs[71:74], refs[74:77], refs[77:80], *refs[80:])

    f, t = lax.axis_index("fs"), lax.axis_index("tp")
    zs = tp // 2
    z, c = t // 2, lax.rem(t, 2)
    mate = 2 * z + 1 - c
    half = feat.shape[0]
    width = feat.shape[1]
    rows_dev = master[0].shape[0]
    rank = proj[0].shape[0]
    rb = rank // n
    piece = half // PIECES
    count = 3 * PIECES
    sends = []

    def remote(src, dst, ssem, rsem, **dev):
        return pltpu.make_async_remote_copy(
            src_ref=src, dst_ref=dst, send_sem=ssem, recv_sem=rsem, device_id=dev, device_id_type=MESH
        )

    def load(src, dst, i):
        cp = pltpu.make_async_copy(src, dst, load_sem.at[i])
        cp.start()
        return cp

    my_half = pl.multiple_of(c * half, half)
    mate_half = pl.multiple_of((1 - c) * half, half)
    loads = [load(feat_in.at[pl.ds(my_half, half)], feat, 0)]
    loads += [load(basis_in[k], basis[k], 1 + k) for k in range(3)]
    loads += [load(cot_in[k], cot[k], 4 + k) for k in range(3)]
    loads += [load(first_in[k], first[k], 7 + k) for k in range(3)]
    loads += [load(second_in[k], second[k], 10 + k) for k in range(3)]
    loads += [load(master_in[k], master[k], 13 + k) for k in range(3)]

    barrier = pltpu.get_barrier_semaphore()
    for d in range(1, n):
        pl.semaphore_signal(barrier, inc=1, device_id={"fs": lax.rem(f + d, n)}, device_id_type=MESH)
    for d in range(1, tp):
        pl.semaphore_signal(barrier, inc=1, device_id={"tp": lax.rem(t + d, tp)}, device_id_type=MESH)
    pl.semaphore_wait(barrier, n + tp - 2)

    share = remote(feat_in.at[pl.ds(mate_half, half)], fsib, sib_send.at[3], sib_recv.at[3], tp=mate)
    share.start()

    @pl.when(z == 0)
    def _():
        up_in[...] = jnp.zeros_like(up_in)

    @pl.when(z == zs - 1)
    def _():
        dn_in[...] = jnp.zeros_like(dn_in)

    for cp in loads[:4]:
        cp.wait()
    mine = pl.ds(pl.multiple_of(t * width, width), width)
    theirs = pl.ds(pl.multiple_of(mate * width, width), width)
    share.wait()
    for k in range(3):
        own = jnp.dot(feat[...], basis[k][mine, :], preferred_element_type=F32)
        own += jnp.dot(fsib[...], basis[k][theirs, :], preferred_element_type=F32)
        for j in range(PIECES):
            parts[k * PIECES + j] = own[j * piece : (j + 1) * piece]

    def hop(j, has_src, has_dst, src_in, snd, lane, to):
        @pl.when((j >= 0) & (j < count))
        def _():
            jj = jnp.clip(j, 0, count - 1)
            copy = remote(snd.at[jj], src_in.at[jj], z_send.at[lane, jj], z_recv.at[lane, jj], tp=to)

            @pl.when(has_src)
            def _():
                copy.wait_recv()

            @pl.when(has_dst)
            def _():
                snd[jj] = (parts[jj] + src_in[jj].astype(F32)).astype(BF16)
                copy.start()

    above = jnp.minimum(t + 2, tp - 2 + c)
    below = jnp.maximum(t - 2, c)

    def z_step(step):
        hop(step - SKEW * z, z > 0, z < zs - 1, up_in, up_snd, 0, above)
        hop(step - SKEW * (zs - 1 - z), z < zs - 1, z > 0, dn_in, dn_snd, 1, below)

    mate_copy = [remote(tot.at[k], sib.at[k], sib_send.at[k], sib_recv.at[k], tp=mate) for k in range(3)]

    def act_total(k):
        for j in range(PIECES):
            i = k * PIECES + j
            whole = parts[i] + up_in[i].astype(F32) + dn_in[i].astype(F32)
            tot[k, j * piece : (j + 1) * piece, :] = whole.astype(BF16)
        mate_copy[k].start()

    def contract(a, b):
        return lax.dot_general(a, b, (((0,), (0,)), ((), ())), preferred_element_type=F32)

    def rows_of(i):
        return pl.ds(pl.multiple_of(i * rb, rb), rb)

    def rs_copy(k, d):
        peer = lax.rem(f + d, n)
        return remote(proj[k].at[rows_of(peer)], rs_in[k].at[d - 1], rs_send.at[k, d - 1], rs_recv.at[k, d - 1], fs=peer)

    def ag_copy(k, d, whose):
        peer = lax.rem(f + d, n)
        r = direction[k].at[rows_of(whose)]
        return remote(r, r, ag_send.at[k, d - 1], ag_recv.at[k, d - 1], fs=peer)

    def sq_copy(k, d, whose):
        peer = lax.rem(t + d, tp)
        r = sums.at[k, whose]
        return remote(r, r, sq_send.at[k, d - 1], sq_recv.at[k, d - 1], tp=peer)

    def act_project(k):
        loads[4 + k].wait()
        acc = contract(tot[k], cot[k][pl.ds(my_half, half), :])
        mate_copy[k].wait_recv()
        proj[k][...] = acc + contract(sib[k], cot[k][pl.ds(mate_half, half), :])
        for d in range(1, n):
            rs_copy(k, d).start()

    def store(src, dst, k, i):
        cp = pltpu.make_async_copy(src, dst, store_sem.at[k, i])
        cp.start()
        sends.append(cp.wait)

    def act_moment(k):
        loads[7 + k].wait()
        loads[10 + k].wait()
        r = proj[k][rows_of(f), :]
        for d in range(1, n):
            rs_copy(k, d).wait_recv()
            r = r + rs_in[k][d - 1]
        a = 0.8 * first[k][...] + 0.2 * r
        b = 0.9 * second[k][...] + 0.1 * r * r
        fir[k][...] = a
        sec[k][...] = b
        direction[k][rows_of(f), :] = a / jnp.sqrt(b)
        for d in range(1, n):
            ag_copy(k, d, f).start()
        store(fir[k], fir_out[k], k, 0)
        store(sec[k], sec_out[k], k, 1)

    rows = pl.ds(pl.multiple_of(f * rows_dev, rows_dev), rows_dev)

    def act_direction(k):
        for d in range(1, n):
            ag_copy(k, d, lax.rem(f - d + n, n)).wait_recv()
        whole = direction[k][...]
        sums[k, t] = jnp.full((8, 128), jnp.sum(whole * whole), F32)
        for d in range(1, tp):
            sq_copy(k, d, t).start()
        high = whole.astype(BF16)
        low = (whole - high.astype(F32)).astype(BF16)
        base = basis[k][rows, :]
        upd[k][...] = jnp.dot(
            jnp.concatenate([base, base], axis=1),
            jnp.concatenate([high, low], axis=0),
            preferred_element_type=F32,
        )

    hrow = rows_dev // 2

    def block(k, owner, h):
        return cop[k].at[pl.ds(pl.multiple_of(owner * rows_dev + h * hrow, hrow), hrow)]

    def out_block(k, owner, h):
        return cop_out[k].at[pl.ds(pl.multiple_of(owner * rows_dev + h * hrow, hrow), hrow)]

    x_peer = f + 1 - 2 * lax.rem(f, 2)
    y_peer = lax.rem(f + 2, 4)
    diag = lax.rem(x_peer + 2, 4)

    def bulk(k, lane, owner, h, to):
        b = block(k, owner, h)
        return remote(b, b, bulk_send.at[k, lane], bulk_recv.at[k, lane], fs=to)

    def act_finish(k):
        loads[13 + k].wait()
        for d in range(1, tp):
            sq_copy(k, d, lax.rem(t - d + tp, tp)).wait_recv()
        total = jnp.sum(sums[k], axis=0)[0:1, 0:1]
        entries = rank * upd[k].shape[1] * tp
        scale = lax.rsqrt(total / entries + 1e-06)
        update = upd[k][...] * scale
        upd[k][...] = update
        new = master[k][...] - 0.05 * update
        mas[k][...] = new
        cop[k][rows, :] = new.astype(BF16)
        if n == 4:
            for h in range(2):
                bulk(k, h, f, h, x_peer).start()
                bulk(k, 3 - h, f, 1 - h, y_peer).start()
        else:
            for d in range(1, n):
                for h in range(2):
                    bulk(k, 2 * (d - 1) + h, f, h, lax.rem(f + d, n)).start()
        store(upd[k], upd_out[k], k, 2)
        store(mas[k], mas_out[k], k, 3)
        for h in range(2):
            store(block(k, f, h), out_block(k, f, h), k, 4 + h)

    def act_forward(k):
        if n == 4:
            bulk(k, 0, x_peer, 0, x_peer).wait_recv()
            bulk(k, 4, x_peer, 0, y_peer).start()
            bulk(k, 3, y_peer, 1, y_peer).wait_recv()
            bulk(k, 5, y_peer, 1, x_peer).start()
            store(block(k, x_peer, 0), out_block(k, x_peer, 0), k, 6)
            store(block(k, y_peer, 1), out_block(k, y_peer, 1), k, 7)

    def act_arrive(k):
        if n == 4:
            for i, (lane, owner, h) in enumerate(((1, x_peer, 1), (2, y_peer, 0), (4, diag, 0), (5, diag, 1))):
                bulk(k, lane, owner, h, x_peer).wait_recv()
                store(block(k, owner, h), out_block(k, owner, h), k, 8 + i)
        else:
            for d in range(1, n):
                for h in range(2):
                    owner = lax.rem(f - d + n, n)
                    lane = 2 * (d - 1) + h
                    bulk(k, lane, owner, h, owner).wait_recv()
                    store(block(k, owner, h), out_block(k, owner, h), k, 6 + lane)

    todo = {}
    for k in range(3):
        base = (k + 1) * PIECES - 1 + SKEW * (zs - 1)
        for after, act in ((0, act_total), (1, act_project), (3, act_moment), (5, act_direction), (7, act_finish), (12, act_forward)):
            todo.setdefault(base + after, []).append((act, k))
    steps = count + SKEW * (zs - 1)
    for step in range(max(max(todo) + 1, steps)):
        if step < steps:
            z_step(step)
        for act, k in todo.get(step, ()):
            act(k)
    for k in range(3):
        act_arrive(k)

    for wait in sends:
        wait()
    for k in range(3):
        mate_copy[k].wait_send()
        for d in range(1, n):
            rs_copy(k, d).wait_send()
            ag_copy(k, d, f).wait_send()
        for d in range(1, tp):
            sq_copy(k, d, t).wait_send()
        if n == 4:
            for h in range(2):
                bulk(k, h, f, h, x_peer).wait_send()
                bulk(k, 3 - h, f, 1 - h, y_peer).wait_send()
            bulk(k, 4, x_peer, 0, y_peer).wait_send()
            bulk(k, 5, y_peer, 1, x_peer).wait_send()
        else:
            for d in range(1, n):
                for h in range(2):
                    bulk(k, 2 * (d - 1) + h, f, h, lax.rem(f + d, n)).wait_send()
    for j in range(count):
        @pl.when(z < zs - 1)
        def _():
            remote(up_snd.at[j], up_in.at[j], z_send.at[0, j], z_recv.at[0, j], tp=above).wait_send()

        @pl.when(z > 0)
        def _():
            remote(dn_snd.at[j], dn_in.at[j], z_send.at[1, j], z_recv.at[1, j], tp=below).wait_send()


def shards(n, tp, *args):
    features = args[0]
    cots, bases, masters, firsts, seconds = (args[1 + i : 16 : 5] for i in range(5))
    tokens, width = features.shape
    rank = bases[0].shape[1]
    rows_dev = masters[0].shape[0]
    whole_rows = rows_dev * n
    half = tokens // 2
    count = 3 * PIECES
    piece = half // PIECES
    cols = [a.shape[1] for a in cots]

    outs = []
    for k in range(3):
        outs += [
            jax.ShapeDtypeStruct(masters[k].shape, F32),
            jax.ShapeDtypeStruct(masters[k].shape, F32),
            jax.ShapeDtypeStruct(firsts[k].shape, F32),
            jax.ShapeDtypeStruct(firsts[k].shape, F32),
            jax.ShapeDtypeStruct((whole_rows, cols[k]), BF16),
        ]
    like = lambda arrays: [pltpu.VMEM(a.shape, a.dtype) for a in arrays]
    lanes = 6 if n == 4 else 2 * (n - 1)
    dma = lambda *shape: pltpu.SemaphoreType.DMA(shape)
    scratch = (
        [pltpu.VMEM((half, width), BF16)] * 2
        + like(cots)
        + like(bases)
        + like(masters)
        + like(firsts)
        + like(seconds)
        + [pltpu.VMEM((count, piece, rank), F32)]
        + [pltpu.VMEM((count, piece, rank), BF16)] * 4
        + [pltpu.VMEM((3, half, rank), BF16)] * 2
        + [pltpu.VMEM((rank, w), F32) for w in cols]
        + [pltpu.VMEM((n - 1, rank // n, w), F32) for w in cols]
        + [pltpu.VMEM((rank, w), F32) for w in cols]
        + [pltpu.VMEM((3, tp, 8, 128), F32)]
        + like(masters)
        + like(masters)
        + like(firsts)
        + like(firsts)
        + [pltpu.VMEM((whole_rows, w), BF16) for w in cols]
        + [dma(16), dma(3, 6 + max(6, 2 * (n - 1))), dma(2, count), dma(2, count), dma(4), dma(4)]
        + [dma(3, n - 1)] * 4
        + [dma(3, tp - 1)] * 2
        + [dma(3, lanes)] * 2
    )
    return pl.pallas_call(
        functools.partial(kernel, n, tp),
        out_shape=outs,
        in_specs=[pl.BlockSpec(memory_space=pl.ANY)] * 16,
        out_specs=[pl.BlockSpec(memory_space=pl.ANY)] * 15,
        scratch_shapes=scratch,
        compiler_params=pltpu.CompilerParams(
            collective_id=0, has_side_effects=True, vmem_limit_bytes=60 * 1024 * 1024
        ),
    )(*args)


def solution(mesh):
    split = P("fs", "tp")
    return jax.shard_map(
        functools.partial(shards, mesh.shape["fs"], mesh.shape["tp"]),
        mesh=mesh,
        in_specs=(split,) + (split, P(), split, split, split) * 3,
        out_specs=(split, split, split, split, P(None, "tp")) * 3,
        check_vma=False,
    )
```

```python
import functools

import jax
import jax.numpy as jnp
from jax import lax
from jax.experimental import pallas as pl
from jax.experimental.pallas import tpu as pltpu
from jax.sharding import PartitionSpec as P

MESH = pl.DeviceIdType.MESH
PIECES = 4
SKEW = 2
AFTER = (0, 1, 4, 7, 9, 13)
F32, BF16 = jnp.float32, jnp.bfloat16


def kernel(n, tp, *refs):
    feat_in = refs[0]
    cot_in, basis_in, master_in, first_in, second_in = (refs[1 + i : 16 : 5] for i in range(5))
    upd, mas, fir, sec, cop = (refs[16 + i : 31 : 5] for i in range(5))
    (feat, fsib, cot, basis, master, first, second, parts, up_in, dn_in, up_snd, dn_snd,
     tot, sib, proj, rs_in, direction, sums,
     load_sem, z_send, z_recv, sib_send, sib_recv, rs_send, rs_recv,
     ag_send, ag_recv, sq_send, sq_recv, bulk_send, bulk_recv) = (
        refs[31], refs[32], refs[33:36], refs[36:39], refs[39:42], refs[42:45], refs[45:48],
        *refs[48:53], refs[53], refs[54], refs[55:58], refs[58:61], refs[61:64], refs[64],
        *refs[65:])

    f, t = lax.axis_index("fs"), lax.axis_index("tp")
    zs = tp // 2
    z, c = t // 2, lax.rem(t, 2)
    mate = 2 * z + 1 - c
    half = feat.shape[0]
    width = feat.shape[1]
    rows_dev = master[0].shape[0]
    rank = proj[0].shape[0]
    rb = rank // n
    piece = half // PIECES
    count = 3 * PIECES

    def remote(src, dst, ssem, rsem, **dev):
        return pltpu.make_async_remote_copy(
            src_ref=src, dst_ref=dst, send_sem=ssem, recv_sem=rsem, device_id=dev, device_id_type=MESH
        )

    def load(src, dst, i):
        cp = pltpu.make_async_copy(src, dst, load_sem.at[i])
        cp.start()
        return cp

    my_half = pl.multiple_of(c * half, half)
    mate_half = pl.multiple_of((1 - c) * half, half)
    loads = [load(feat_in.at[pl.ds(my_half, half)], feat, 0)]
    loads += [load(basis_in[k], basis[k], 1 + k) for k in range(3)]
    loads += [load(cot_in[k], cot[k], 4 + k) for k in range(3)]
    loads += [load(first_in[k], first[k], 7 + k) for k in range(3)]
    loads += [load(second_in[k], second[k], 10 + k) for k in range(3)]
    loads += [load(master_in[k], master[k], 13 + k) for k in range(3)]

    barrier = pltpu.get_barrier_semaphore()
    for d in range(1, n):
        pl.semaphore_signal(barrier, inc=1, device_id={"fs": lax.rem(f + d, n)}, device_id_type=MESH)
    for d in range(1, tp):
        pl.semaphore_signal(barrier, inc=1, device_id={"tp": lax.rem(t + d, tp)}, device_id_type=MESH)
    pl.semaphore_wait(barrier, n + tp - 2)

    share = remote(feat_in.at[pl.ds(mate_half, half)], fsib, sib_send.at[3], sib_recv.at[3], tp=mate)
    share.start()

    @pl.when(z == 0)
    def _():
        up_in[...] = jnp.zeros_like(up_in)

    @pl.when(z == zs - 1)
    def _():
        dn_in[...] = jnp.zeros_like(dn_in)

    for cp in loads[:4]:
        cp.wait()
    mine = pl.ds(pl.multiple_of(t * width, width), width)
    theirs = pl.ds(pl.multiple_of(mate * width, width), width)
    share.wait()
    for k in range(3):
        own = jnp.dot(feat[...], basis[k][mine, :], preferred_element_type=F32)
        own += jnp.dot(fsib[...], basis[k][theirs, :], preferred_element_type=F32)
        for j in range(PIECES):
            parts[k * PIECES + j] = own[j * piece : (j + 1) * piece]

    def hop(j, has_src, has_dst, src_in, snd, lane, to):
        @pl.when((j >= 0) & (j < count))
        def _():
            jj = jnp.clip(j, 0, count - 1)
            copy = remote(snd.at[jj], src_in.at[jj], z_send.at[lane, jj], z_recv.at[lane, jj], tp=to)

            @pl.when(has_src)
            def _():
                copy.wait_recv()

            @pl.when(has_dst)
            def _():
                snd[jj] = (parts[jj] + src_in[jj].astype(F32)).astype(BF16)
                copy.start()

    above = jnp.minimum(t + 2, tp - 2 + c)
    below = jnp.maximum(t - 2, c)

    def z_step(step):
        hop(step - SKEW * z, z > 0, z < zs - 1, up_in, up_snd, 0, above)
        hop(step - SKEW * (zs - 1 - z), z < zs - 1, z > 0, dn_in, dn_snd, 1, below)

    mate_copy = [remote(tot.at[k], sib.at[k], sib_send.at[k], sib_recv.at[k], tp=mate) for k in range(3)]

    def act_total(k):
        for j in range(PIECES):
            i = k * PIECES + j
            whole = parts[i] + up_in[i].astype(F32) + dn_in[i].astype(F32)
            tot[k, j * piece : (j + 1) * piece, :] = whole.astype(BF16)
        mate_copy[k].start()

    def contract(a, b):
        return lax.dot_general(a, b, (((0,), (0,)), ((), ())), preferred_element_type=F32)

    def rows_of(i):
        return pl.ds(pl.multiple_of(i * rb, rb), rb)

    def rs_copy(k, d):
        peer = lax.rem(f + d, n)
        return remote(proj[k].at[rows_of(peer)], rs_in[k].at[d - 1], rs_send.at[k, d - 1], rs_recv.at[k, d - 1], fs=peer)

    def ag_copy(k, d, whose):
        peer = lax.rem(f + d, n)
        r = direction[k].at[rows_of(whose)]
        return remote(r, r, ag_send.at[k, d - 1], ag_recv.at[k, d - 1], fs=peer)

    def sq_copy(k, d, whose):
        peer = lax.rem(t + d, tp)
        r = sums.at[k, whose]
        return remote(r, r, sq_send.at[k, d - 1], sq_recv.at[k, d - 1], tp=peer)

    def act_project(k):
        loads[4 + k].wait()
        acc = contract(tot[k], cot[k][pl.ds(my_half, half), :])
        mate_copy[k].wait_recv()
        proj[k][...] = acc + contract(sib[k], cot[k][pl.ds(mate_half, half), :])
        for d in range(1, n):
            rs_copy(k, d).start()

    def act_moment(k):
        loads[7 + k].wait()
        loads[10 + k].wait()
        r = proj[k][rows_of(f), :]
        for d in range(1, n):
            rs_copy(k, d).wait_recv()
            r = r + rs_in[k][d - 1]
        a = 0.8 * first[k][...] + 0.2 * r
        b = 0.9 * second[k][...] + 0.1 * r * r
        fir[k][...] = a
        sec[k][...] = b
        direction[k][rows_of(f), :] = a / jnp.sqrt(b)
        for d in range(1, n):
            ag_copy(k, d, f).start()

    rows = pl.ds(pl.multiple_of(f * rows_dev, rows_dev), rows_dev)

    def act_direction(k):
        for d in range(1, n):
            ag_copy(k, d, lax.rem(f - d + n, n)).wait_recv()
        whole = direction[k][...]
        sums[k, t] = jnp.full((8, 128), jnp.sum(whole * whole), F32)
        for d in range(1, tp):
            sq_copy(k, d, t).start()
        high = whole.astype(BF16)
        low = (whole - high.astype(F32)).astype(BF16)
        base = basis[k][rows, :]
        upd[k][...] = jnp.dot(
            jnp.concatenate([base, base], axis=1),
            jnp.concatenate([high, low], axis=0),
            preferred_element_type=F32,
        )

    hrow = rows_dev // 2

    def block(k, owner, h):
        return cop[k].at[pl.ds(pl.multiple_of(owner * rows_dev + h * hrow, hrow), hrow)]

    x_peer = f + 1 - 2 * lax.rem(f, 2)
    y_peer = lax.rem(f + 2, 4)
    diag = lax.rem(x_peer + 2, 4)

    def bulk(k, lane, owner, h, to):
        b = block(k, owner, h)
        return remote(b, b, bulk_send.at[k, lane], bulk_recv.at[k, lane], fs=to)

    def act_finish(k):
        loads[13 + k].wait()
        for d in range(1, tp):
            sq_copy(k, d, lax.rem(t - d + tp, tp)).wait_recv()
        total = jnp.sum(sums[k], axis=0)[0:1, 0:1]
        entries = rank * upd[k].shape[1] * tp
        scale = lax.rsqrt(total / entries + 1e-06)
        update = upd[k][...] * scale
        upd[k][...] = update
        new = master[k][...] - 0.05 * update
        mas[k][...] = new
        cop[k][rows, :] = new.astype(BF16)
        if n == 4:
            for h in range(2):
                bulk(k, h, f, h, x_peer).start()
                bulk(k, 3 - h, f, 1 - h, y_peer).start()
        else:
            for d in range(1, n):
                for h in range(2):
                    bulk(k, 2 * (d - 1) + h, f, h, lax.rem(f + d, n)).start()

    def act_forward(k):
        if n == 4:
            bulk(k, 0, x_peer, 0, x_peer).wait_recv()
            bulk(k, 4, x_peer, 0, y_peer).start()
            bulk(k, 3, y_peer, 1, y_peer).wait_recv()
            bulk(k, 5, y_peer, 1, x_peer).start()

    def act_arrive(k):
        if n == 4:
            for i, (lane, owner, h) in enumerate(((1, x_peer, 1), (2, y_peer, 0), (4, diag, 0), (5, diag, 1))):
                bulk(k, lane, owner, h, x_peer).wait_recv()
        else:
            for d in range(1, n):
                for h in range(2):
                    owner = lax.rem(f - d + n, n)
                    lane = 2 * (d - 1) + h
                    bulk(k, lane, owner, h, owner).wait_recv()

    todo = {}
    for k in range(3):
        base = (k + 1) * PIECES - 1 + SKEW * (zs - 1)
        for after, act in zip(AFTER, (act_total, act_project, act_moment, act_direction, act_finish, act_forward)):
            todo.setdefault(base + after, []).append((act, k))
    steps = count + SKEW * (zs - 1)
    for step in range(max(max(todo) + 1, steps)):
        if step < steps:
            z_step(step)
        for act, k in sorted(todo.get(step, ()), key=lambda item: -item[1]):
            act(k)
    for k in range(3):
        act_arrive(k)

    for k in range(3):
        mate_copy[k].wait_send()
        for d in range(1, n):
            rs_copy(k, d).wait_send()
            ag_copy(k, d, f).wait_send()
        for d in range(1, tp):
            sq_copy(k, d, t).wait_send()
        if n == 4:
            for h in range(2):
                bulk(k, h, f, h, x_peer).wait_send()
                bulk(k, 3 - h, f, 1 - h, y_peer).wait_send()
            bulk(k, 4, x_peer, 0, y_peer).wait_send()
            bulk(k, 5, y_peer, 1, x_peer).wait_send()
        else:
            for d in range(1, n):
                for h in range(2):
                    bulk(k, 2 * (d - 1) + h, f, h, lax.rem(f + d, n)).wait_send()
    for j in range(count):
        @pl.when(z < zs - 1)
        def _():
            remote(up_snd.at[j], up_in.at[j], z_send.at[0, j], z_recv.at[0, j], tp=above).wait_send()

        @pl.when(z > 0)
        def _():
            remote(dn_snd.at[j], dn_in.at[j], z_send.at[1, j], z_recv.at[1, j], tp=below).wait_send()


def shards(n, tp, *args):
    features = args[0]
    cots, bases, masters, firsts, seconds = (args[1 + i : 16 : 5] for i in range(5))
    tokens, width = features.shape
    rank = bases[0].shape[1]
    rows_dev = masters[0].shape[0]
    whole_rows = rows_dev * n
    half = tokens // 2
    count = 3 * PIECES
    piece = half // PIECES
    cols = [a.shape[1] for a in cots]

    outs = []
    for k in range(3):
        outs += [
            pltpu.VMEM(masters[k].shape, F32),
            pltpu.VMEM(masters[k].shape, F32),
            pltpu.VMEM(firsts[k].shape, F32),
            pltpu.VMEM(firsts[k].shape, F32),
            pltpu.VMEM((whole_rows, cols[k]), BF16),
        ]
    like = lambda arrays: [pltpu.VMEM(a.shape, a.dtype) for a in arrays]
    lanes = 6 if n == 4 else 2 * (n - 1)
    dma = lambda *shape: pltpu.SemaphoreType.DMA(shape)
    scratch = (
        [pltpu.VMEM((half, width), BF16)] * 2
        + like(cots)
        + like(bases)
        + like(masters)
        + like(firsts)
        + like(seconds)
        + [pltpu.VMEM((count, piece, rank), F32)]
        + [pltpu.VMEM((count, piece, rank), BF16)] * 4
        + [pltpu.VMEM((3, half, rank), BF16)] * 2
        + [pltpu.VMEM((rank, w), F32) for w in cols]
        + [pltpu.VMEM((n - 1, rank // n, w), F32) for w in cols]
        + [pltpu.VMEM((rank, w), F32) for w in cols]
        + [pltpu.VMEM((3, tp, 8, 128), F32)]
        + [dma(16), dma(2, count), dma(2, count), dma(4), dma(4)]
        + [dma(3, n - 1)] * 4
        + [dma(3, tp - 1)] * 2
        + [dma(3, lanes)] * 2
    )
    return pl.pallas_call(
        functools.partial(kernel, n, tp),
        out_shape=outs,
        in_specs=[pl.BlockSpec(memory_space=pltpu.HBM)] * 16,
        out_specs=[pl.BlockSpec(memory_space=pltpu.VMEM)] * 15,
        scratch_shapes=scratch,
        compiler_params=pltpu.CompilerParams(
            collective_id=0, has_side_effects=True, vmem_limit_bytes=54 * 1024 * 1024
        ),
    )(*args)


def solution(mesh):
    split = P("fs", "tp")
    return jax.shard_map(
        functools.partial(shards, mesh.shape["fs"], mesh.shape["tp"]),
        mesh=mesh,
        in_specs=(split,) + (split, P(), split, split, split) * 3,
        out_specs=(split, split, split, split, P(None, "tp")) * 3,
        check_vma=False,
    )
```
